32 devices in a mesh: kv: 8 (over z, y), tp: 4 (over x, core).
Axes of the slice: x: 2, y: 2, z: 4, core: 2. Of those that a mesh axis runs over, the one named last changes fastest.
Arguments:
- tokens: bfloat16 [6144, 2048], P('kv'), may hold values from -6 to 6
- w_query: bfloat16 [2048, 4096], P(None, 'tp'), may hold values from -3.1819805 to 3.1819805
- w_latent: bfloat16 [2048, 256], replicated, may hold values from -0.13258252 to 0.13258252
- latent_gain: float32 [256], replicated, may hold values from 0.1 to 1.9
- w_output: bfloat16 [4096, 2048], P('tp'), may hold values from -2 to 2
- chosen: int32 [96, 32], P('kv'), may hold values from -1 to 95, as said below
Outputs:
- attended: bfloat16 [6144, 2048], P(('kv', 'tp'))
- log_total: float32 [6144, 16], P('kv', 'tp')
The draws below stay inside these ranges and needn't reach their ends.
Inputs may be any that keep to these rules, and one draw needn't show every extreme that they name: `chosen`: row g names blocks at or before block g, no block twice; entry 0 is g itself; entries -1 name nothing and stand after the others. The 12 rows of one device together name exactly 2 distinct blocks of every earlier device's positions and none of a later device's.
All inputs are finite; a program needn't handle non-finite values.
Results may differ from the reference program's by a relative error of at most 0.01.
Values may be sent and summed in bfloat16 or wider, within the bound.
No kernel may reach another device: no remote copies, remote signals or barrier semaphores. Data moves between devices by JAX's collectives and lax.ppermute only.
A program may use at most 192 MiB of HBM per device.

```python
import math
import jax
import jax.numpy as jnp
from jax import lax

D = 2048
HEADS = 16
R = 256
BLK = 64
NSEL = 32
CAP = 2
TOK_DEV = 768
SEQ = 6144
N_TP = 4


def latent_base(key):
    return jax.random.truncated_normal(jax.random.fold_in(key, 7), -6.0, 6.0, (D, R), jnp.float32) * D ** (-0.5)


def draw_w_latent(key, part):
    return latent_base(key).astype(jnp.bfloat16)


def draw_w_query(key, part):
    drawn = jax.random.truncated_normal(jax.random.fold_in(key, 11), -6.0, 6.0, (D, HEADS, R), jnp.float32) * D ** (-0.5)
    return drawn.reshape(D, HEADS * R).astype(jnp.bfloat16)


def draw_chosen(key, part):
    per_device = TOK_DEV // BLK
    block_count = SEQ // BLK
    devices = SEQ // TOK_DEV
    key_offer = jax.random.fold_in(key, 21)
    key_popular = jax.random.fold_in(key, 22)
    key_noise = jax.random.fold_in(key, 23)
    offer_raw = jax.random.randint(key_offer, (devices, devices, per_device), 0, 1 << 16)
    offer_score = offer_raw * per_device + jnp.arange(per_device, dtype=jnp.int32)
    offer_rank = jnp.argsort(jnp.argsort(-offer_score, axis=2), axis=2)
    offered = offer_rank < CAP
    popular = jax.random.randint(key_popular, (devices,), 0, 4)
    blocks = jnp.arange(block_count, dtype=jnp.int32)
    owner = blocks // per_device
    local_part = blocks % per_device
    dev_row = owner[:, None]
    own_col = owner[None, :]
    local_row = local_part[:, None]
    is_offered = offered[dev_row, own_col, local_part[None, :]]
    rank_here = offer_rank[dev_row, own_col, local_part[None, :]]
    earlier = blocks[None, :] <= blocks[:, None]
    other_ok = (own_col < dev_row) & is_offered
    allowed = (own_col == dev_row) & earlier | other_ok
    forced = other_ok & ((own_col * CAP + rank_here) % per_device == local_row)
    hot = (own_col == 0) | (own_col == dev_row - 1) | (own_col == dev_row - devices // 2)
    bias = jnp.where(blocks[None, :] == blocks[:, None], 40, jnp.where(forced, 30, jnp.where(own_col == dev_row, 8, jnp.where(hot, 20, 2 * popular[own_col]))))
    noise = jax.random.randint(key_noise, (block_count, block_count), 0, 4096)
    score = (bias * 4096 + noise) * block_count + blocks[None, :]
    score = jnp.where(allowed, score, -1 - blocks[None, :])
    values, picked = lax.top_k(score, NSEL)
    return jnp.where(values >= 0, picked, -1).astype(jnp.int32)


def steps_of(stream_key, shape, split, smallest, high):
    def one(dim, blocks):
        steps = jax.random.uniform(jax.random.fold_in(jax.random.fold_in(stream_key, 6), dim), (blocks,), jnp.float32, smallest / len(split), high / len(split))
        return jnp.repeat(jnp.exp(steps), shape[dim] // blocks).reshape((-1,) + (1,) * (len(shape) - dim - 1))

    gain = one(*split[0])
    for cut in split[1:]:
        gain = gain * one(*cut)
    return gain


def normal_values(key, shape, scale, most, shards=(), kind=jnp.bfloat16):
    values = scale * jax.random.normal(key, shape, jnp.float32)
    if shards:
        values = values * steps_of(key, shape, shards, -0.22, 0.18)
    return jnp.clip(values, -most, most).astype(kind)


def setup_inputs(seed: int = 0) -> dict:
    key_of = jax.random.split(jax.random.key(seed), 7)
    tokens = normal_values(key_of[0], (SEQ, D), 1.0, 6.0, ((0, 8),))
    w_query = draw_w_query(jax.random.fold_in(key_of[6], 71), 0)
    w_latent = draw_w_latent(jax.random.fold_in(key_of[6], 71), 0)
    latent_gain = jnp.clip(1.0 + 0.18 * jax.random.normal(key_of[3], (R,), jnp.float32), 0.1, 1.9)
    w_output = normal_values(key_of[4], (HEADS * R, D), 8 ** -0.5, 2.0, ((0, 4),))
    chosen = draw_chosen(jax.random.fold_in(key_of[6], 71), 0)
    return {"tokens": tokens, "w_query": w_query, "w_latent": w_latent, "latent_gain": latent_gain, "w_output": w_output, "chosen": chosen}


epsilon = 1e-06

def latents_of(tokens, w_latent, latent_gain):
    projected = jnp.dot(tokens, w_latent, preferred_element_type=jnp.float32)
    inv_rms = lax.rsqrt(lax.optimization_barrier(jnp.mean(projected * projected, axis=-1, keepdims=True)) + epsilon)
    return (projected * inv_rms * latent_gain).astype(jnp.bfloat16)

def attend(query_part, key_rows, picked, query_blocks, blk_len, score_scale):
    group_size, picks_each = picked.shape
    offsets = jnp.arange(blk_len, dtype=jnp.int32)
    key_pos = (picked[:, :, None] * blk_len + offsets[None, None, :]).reshape(group_size, picks_each * blk_len)
    usable = jnp.repeat(picked >= 0, blk_len, axis=1)
    query_pos = query_blocks[:, None] * blk_len + offsets[None, :]
    allowed = usable[:, None, :] & (key_pos[:, None, :] <= query_pos[:, :, None])
    scores = jnp.einsum('gqhr,gkr->ghqk', query_part.astype(jnp.float32), key_rows.astype(jnp.float32)) * score_scale
    scores = jnp.where(allowed[:, None, :, :], scores, -jnp.inf)
    peak_score = lax.optimization_barrier(jnp.max(scores, axis=3, keepdims=True))
    raised = jnp.exp(scores - peak_score)
    total_mass = lax.optimization_barrier(jnp.sum(raised, axis=3))
    weights = raised.astype(jnp.bfloat16)
    summed = jnp.einsum('ghqk,gkr->gqhr', weights.astype(jnp.float32), key_rows.astype(jnp.float32))
    mass_t = jnp.transpose(total_mass, (0, 2, 1))
    heads_out = (summed / mass_t[..., None]).astype(jnp.bfloat16)
    log_part = jnp.transpose(peak_score[..., 0], (0, 2, 1)) + jnp.log(mass_t)
    return (heads_out, log_part)

def reference(tokens, w_query, w_latent, latent_gain, w_output, chosen):
    seq_len, width = tokens.shape
    lat_rank = w_latent.shape[1]
    head_count = w_query.shape[1] // lat_rank
    block_count, picks_each = chosen.shape
    blk_len = seq_len // block_count
    latent = latents_of(tokens, w_latent, latent_gain)
    queries = jnp.dot(tokens, w_query, preferred_element_type=jnp.float32).astype(jnp.bfloat16)
    queries = queries.reshape(block_count, blk_len, head_count, lat_rank)
    key_table = latent.reshape(block_count, blk_len, lat_rank)
    group_size = math.gcd(block_count, 8)
    score_scale = lat_rank ** (-0.5)

    def one_group(offset):
        picked = lax.dynamic_slice_in_dim(chosen, offset, group_size, 0)
        query_part = lax.dynamic_slice_in_dim(queries, offset, group_size, 0)
        key_rows = jnp.take(key_table, jnp.maximum(picked, 0), axis=0).reshape(group_size, picks_each * blk_len, lat_rank)
        query_blocks = offset + jnp.arange(group_size, dtype=jnp.int32)
        return attend(query_part, key_rows, picked, query_blocks, blk_len, score_scale)
    group_starts = jnp.arange(0, block_count, group_size, dtype=jnp.int32)
    heads_out, log_total = lax.map(one_group, group_starts)
    heads_flat = heads_out.reshape(seq_len, head_count * lat_rank)
    log_total = log_total.reshape(seq_len, head_count)
    group_cols = head_count // N_TP * lat_rank
    attended = jnp.zeros((seq_len, width), jnp.float32)
    for group_index in range(N_TP):
        low = group_index * group_cols
        partial_value = jnp.dot(heads_flat[:, low:low + group_cols], w_output[low:low + group_cols], preferred_element_type=jnp.float32)
        attended = attended + lax.optimization_barrier(partial_value.astype(jnp.bfloat16)).astype(jnp.float32)
    return (attended.astype(jnp.bfloat16), log_total)
```

```python
import functools
import math

import jax
import jax.numpy as jnp
from jax import lax
from jax.experimental import pallas as pl
from jax.experimental.pallas import tpu as pltpu
from jax.sharding import PartitionSpec as P

CAP = 2
NEG = -1e30
epsilon = 1e-06
VMEM = pltpu.VMEM


def latent_kernel(tok_ref, w_ref, gain_ref, out_ref):
    projected = jnp.dot(tok_ref[...], w_ref[...], preferred_element_type=jnp.float32)
    inv_rms = lax.rsqrt(jnp.mean(projected * projected, axis=-1, keepdims=True) + epsilon)
    out_ref[...] = (projected * inv_rms * gain_ref[...]).astype(out_ref.dtype)


def latents_of(tokens, w_latent, latent_gain):
    rows, width = tokens.shape
    rank = w_latent.shape[1]
    tile = math.gcd(rows, 256)
    return pl.pallas_call(
        latent_kernel,
        grid=(rows // tile,),
        in_specs=[
            pl.BlockSpec((tile, width), lambda i: (i, 0)),
            pl.BlockSpec((width, rank), lambda i: (0, 0)),
            pl.BlockSpec((1, rank), lambda i: (0, 0)),
        ],
        out_specs=pl.BlockSpec((tile, rank), lambda i: (i, 0)),
        out_shape=jax.ShapeDtypeStruct((rows, rank), jnp.bfloat16),
        cost_estimate=pl.CostEstimate(
            flops=2 * rows * width * rank, bytes_accessed=2 * rows * width, transcendentals=rows
        ),
        name="latents",
    )(tokens, w_latent, latent_gain.reshape(1, rank))


def query_kernel(core_ref, tok_ref, w_ref, out_ref):
    m, _, tile, width = tok_ref.shape
    rows = tok_ref[...].reshape(m * tile, width)
    out = jnp.dot(rows, w_ref[...], preferred_element_type=jnp.float32)
    out_ref[...] = out.astype(out_ref.dtype)


def queries_of(core, tokens4, w_query, rank):
    m, pair, tile, width = tokens4.shape
    cols = w_query.shape[1]
    return pl.pallas_call(
        query_kernel,
        grid_spec=pltpu.PrefetchScalarGridSpec(
            num_scalar_prefetch=1,
            grid=(cols // rank,),
            in_specs=[
                pl.BlockSpec((m, 1, tile, width), lambda i, core: (0, core[0], 0, 0)),
                pl.BlockSpec((width, rank), lambda i, core: (0, i)),
            ],
            out_specs=pl.BlockSpec((m * tile, rank), lambda i, core: (0, i)),
        ),
        out_shape=jax.ShapeDtypeStruct((m * tile, cols), jnp.bfloat16),
        cost_estimate=pl.CostEstimate(
            flops=2 * m * tile * width * cols,
            bytes_accessed=2 * width * cols,
            transcendentals=0,
        ),
        name="queries",
    )(core, tokens4, w_query)


def pick_kernel(meta_ref, lat_ref, out_ref):
    for i in range(out_ref.shape[0]):
        out_ref[i] = lat_ref[meta_ref[i], meta_ref[out_ref.shape[0]]]


def pick_halves(meta, latent4, count):
    _, _, half, rank = latent4.shape
    return pl.pallas_call(
        pick_kernel,
        grid_spec=pltpu.PrefetchScalarGridSpec(
            num_scalar_prefetch=1,
            in_specs=[pl.BlockSpec(memory_space=VMEM)],
            out_specs=pl.BlockSpec(memory_space=VMEM),
        ),
        out_shape=jax.ShapeDtypeStruct((count, half, rank), latent4.dtype),
        name="pick",
    )(meta, latent4)


def attend_kernel(
    scale, meta_ref, qa_ref, qb_ref, own_ref, r1_ref, r2_ref, bias_ref, ho_ref, lse_ref, s_ref, p_ref, bl_ref
):
    blk_len = qa_ref.shape[2]
    rank = own_ref.shape[1]
    heads = qa_ref.shape[3] // rank
    own_len = own_ref.shape[0]
    rem_len = r1_ref.shape[0]
    key_len = own_len + 2 * rem_len
    unit = heads * blk_len
    exp_scale = scale * math.log2(math.e)
    row0 = (meta_ref[1] + pl.program_id(0)) * blk_len
    k_pos = lax.broadcasted_iota(jnp.int32, (blk_len, own_len), 1)
    q_pos = lax.broadcasted_iota(jnp.int32, (blk_len, own_len), 0) + row0
    bl_ref[...] = jnp.where(k_pos <= q_pos, bias_ref[0, :, :own_len], NEG)
    tile = math.gcd(math.gcd(own_len, rem_len), 256)
    parts = []
    base = 0
    for ref in (own_ref, r1_ref, r2_ref):
        for at in range(0, ref.shape[0], tile):
            parts.append((ref, at, base + at))
        base += ref.shape[0]
    for u, q_ref in enumerate((qa_ref, qb_ref)):
        q = jnp.concatenate(
            [q_ref[0, 0, :, h * rank : (h + 1) * rank] for h in range(heads)], axis=0
        )
        for ref, at, col in parts:
            s = lax.dot_general(
                q, ref[at : at + tile, :], (((1,), (1,)), ((), ())), preferred_element_type=jnp.float32
            )
            if col < own_len:
                add = bl_ref[:, col : col + tile][None]
            else:
                add = bias_ref[0, :, col : col + tile][None]
            s = s.reshape(heads, blk_len, tile) + add
            s_ref[u * unit : (u + 1) * unit, col : col + tile] = s.reshape(unit, tile)
    lses = []
    for u in range(2):
        masses = []
        for h in range(heads):
            at = u * unit + h * blk_len
            peak = s_ref[at : at + blk_len, 0:128]
            for col in range(128, key_len, 128):
                peak = jnp.maximum(peak, s_ref[at : at + blk_len, col : col + 128])
            peak = jnp.max(peak, axis=1, keepdims=True)
            mass = jnp.zeros((blk_len, 128), jnp.float32)
            for col in range(0, key_len, 128):
                raised = jnp.exp2((s_ref[at : at + blk_len, col : col + 128] - peak) * exp_scale)
                mass = mass + raised
                p_ref[at : at + blk_len, col : col + 128] = raised.astype(p_ref.dtype)
            mass = jnp.sum(mass, axis=1, keepdims=True)
            masses.append(1.0 / mass)
            lses.append(peak * scale + jnp.log(mass))
        out = jnp.zeros((unit, rank), jnp.float32)
        base = 0
        for ref in (own_ref, r1_ref, r2_ref):
            n = ref.shape[0]
            out = out + jnp.dot(
                p_ref[u * unit : (u + 1) * unit, base : base + n], ref[...], preferred_element_type=jnp.float32
            )
            base += n
        for h in range(heads):
            ho_ref[0, :, (u * heads + h) * rank : (u * heads + h + 1) * rank] = (
                out[h * blk_len : (h + 1) * blk_len] * masses[h]
            ).astype(ho_ref.dtype)
    lse_ref[0] = jnp.concatenate(lses, axis=1)


def attend(meta, qa, qb, latent, r1, r2, bias, first, count, scale):
    _, _, blk_len, cols = qa.shape
    rank = latent.shape[1]
    heads = 2 * cols // rank
    key_len = bias.shape[-1]
    q_spec = pl.BlockSpec((1, 1, blk_len, cols), lambda i, meta: (meta[0], first + i, 0, 0))

    def whole(array):
        return pl.BlockSpec(array.shape, lambda i, meta: (0, 0))

    rows = heads * blk_len
    return pl.pallas_call(
        functools.partial(attend_kernel, scale),
        grid_spec=pltpu.PrefetchScalarGridSpec(
            num_scalar_prefetch=1,
            grid=(count,),
            in_specs=[
                q_spec,
                q_spec,
                whole(latent),
                whole(r1),
                whole(r2),
                pl.BlockSpec((1, 1, key_len), lambda i, meta: (meta[1] + i, 0, 0)),
            ],
            out_specs=[
                pl.BlockSpec((1, blk_len, 2 * cols), lambda i, meta: (i, 0, 0)),
                pl.BlockSpec((1, blk_len, heads), lambda i, meta: (i, 0, 0)),
            ],
            scratch_shapes=[
                VMEM((rows, key_len), jnp.float32),
                VMEM((rows, key_len), jnp.bfloat16),
                VMEM((blk_len, latent.shape[0]), jnp.float32),
            ],
        ),
        out_shape=[
            jax.ShapeDtypeStruct((count, blk_len, 2 * cols), jnp.bfloat16),
            jax.ShapeDtypeStruct((count, blk_len, heads), jnp.float32),
        ],
        cost_estimate=pl.CostEstimate(
            flops=4 * count * rows * key_len * rank,
            bytes_accessed=2 * key_len * rank,
            transcendentals=count * rows * key_len,
        ),
        name="attend",
    )(meta, qa, qb, latent, r1, r2, bias)


def local(tokens, w_query, w_latent, latent_gain, w_output, chosen):
    tok_rows, width = tokens.shape
    rank = w_latent.shape[1]
    heads = w_query.shape[1] // rank
    per_device, picks = chosen.shape
    blk_len = tok_rows // per_device
    half = blk_len // 2
    devices = lax.axis_size("kv")
    n_tp = lax.axis_size("tp")
    m = n_tp // 2
    tile_rows = tok_rows // n_tp
    tile_blocks = tile_rows // blk_len
    mine = lax.axis_index("kv")
    tp = lax.axis_index("tp")
    chip, core = tp // 2, tp % 2
    swap = [(i, i ^ 1) for i in range(n_tp)]

    wq_other = lax.ppermute(w_query, "tp", swap)
    wo_other = lax.ppermute(w_output, "tp", swap)

    flat = chosen.reshape(1, per_device * picks)
    first_id = (jnp.arange(devices, dtype=jnp.int32) * per_device)[:, None]
    of_owner = (flat >= first_id) & (flat < first_id + per_device)
    low = jnp.min(jnp.where(of_owner, flat, devices * per_device), axis=1)
    high = jnp.max(jnp.where(of_owner, flat, -1), axis=1)
    request = jnp.stack([low, high], axis=1)
    asked = lax.all_to_all(request, "kv", split_axis=0, concat_axis=0, tiled=True)

    latent = latents_of(tokens, w_latent, latent_gain)
    tokens4 = tokens.reshape(m, 2, tile_rows, width)
    core1 = core.reshape(1).astype(jnp.int32)
    qa = queries_of(core1, tokens4, w_query, rank)

    local_ids = jnp.clip(asked - mine * per_device, 0, per_device - 1).reshape(devices * CAP)
    pick_meta = jnp.concatenate([local_ids, core1])
    reply = pick_halves(pick_meta, latent.reshape(per_device, 2, half, rank), devices * CAP)
    fetched = lax.all_to_all(
        reply.reshape(devices, CAP, half, rank), "kv", split_axis=0, concat_axis=0, tiled=True
    )
    r1 = fetched.reshape(devices * CAP * half, rank)
    r2 = lax.ppermute(r1, "tp", swap)
    qb = queries_of(core1, tokens4, wq_other, rank)

    earlier = jnp.arange(devices, dtype=jnp.int32) < mine
    slots = jnp.stack(
        [jnp.where(earlier, low, -2), jnp.where(earlier & (high > low), high, -2)], axis=1
    ).reshape(devices * CAP)
    own_ids = mine * per_device + jnp.arange(per_device, dtype=jnp.int32)
    slot_keys = jnp.repeat(slots, half)
    key_ids = jnp.concatenate([jnp.repeat(own_ids, blk_len), slot_keys, slot_keys])
    named = jnp.any(chosen[:, :, None] == key_ids[None, None, :], axis=1)
    bias = jnp.where(named, 0.0, NEG).astype(jnp.float32)[:, None, :]

    qa4 = qa.reshape(m, tile_blocks, blk_len, heads * rank)
    qb4 = qb.reshape(m, tile_blocks, blk_len, heads * rank)
    scale = rank ** (-0.5)

    def work(k, first, count):
        chip_k = (chip + k) % m
        meta = jnp.stack([chip_k, (chip_k * 2 + core) * tile_blocks + first]).astype(jnp.int32)
        ho, lse = attend(meta, qa4, qb4, latent, r1, r2, bias, first, count, scale)
        ho = ho.reshape(count * blk_len, 2 * heads * rank)
        out = jnp.dot(ho[:, : heads * rank], w_output, preferred_element_type=jnp.float32)
        out = out + jnp.dot(ho[:, heads * rank :], wo_other, preferred_element_type=jnp.float32)
        return out, lse.reshape(count * blk_len, 2 * heads)

    splits = [(0, 1), (1, tile_blocks - 1)] if tile_blocks > 1 else [(0, 1)]
    lse_tiles = [None] * m
    arrived = []
    for k in range(1, m):
        to_chip = [(i, (i + 2 * k) % n_tp) for i in range(n_tp)]
        pieces, lses = [], []
        for first, count in splits:
            out, lse = work(k, first, count)
            pieces.append(lax.ppermute(out.astype(jnp.bfloat16), "tp", to_chip))
            lses.append(lse)
        arrived.append(pieces)
        lse_tiles[k] = jnp.concatenate(lses, axis=0)
    total, lse_tiles[0] = work(0, 0, tile_blocks)
    received = [jnp.concatenate(pieces, axis=0).astype(jnp.float32) for pieces in arrived]
    for piece in received:
        total = total + piece
    attended = total.astype(jnp.bfloat16)

    lse = jnp.stack(lse_tiles)
    lse = lax.dynamic_slice_in_dim(jnp.concatenate([lse, lse], axis=0), (m - chip) % m, m, 0)
    theirs = lax.ppermute(lse[..., heads:], "tp", swap)
    ours = lse[..., :heads]
    log_total = jnp.where(
        core == 0, jnp.stack([ours, theirs], axis=1), jnp.stack([theirs, ours], axis=1)
    ).reshape(tok_rows, heads)
    return (attended, log_total)


def solution(mesh):
    placed = (P("kv", None), P(None, "tp"), P(), P(), P("tp", None), P("kv", None))
    return jax.shard_map(
        local,
        mesh=mesh,
        in_specs=placed,
        out_specs=(P(("kv", "tp"), None), P("kv", "tp")),
        check_vma=False,
    )
```

```python
import functools
import math

import jax
import jax.numpy as jnp
from jax import lax
from jax.experimental import pallas as pl
from jax.experimental.pallas import tpu as pltpu
from jax.sharding import PartitionSpec as P


CAP = 2
NEG = -1e30
epsilon = 1e-06
VMEM = pltpu.VMEM
DMA = pltpu.SemaphoreType.DMA
ANY = pl.BlockSpec(memory_space=pltpu.HBM)
ON_CHIP = pl.BlockSpec(memory_space=VMEM)
SCALARS = pl.BlockSpec(memory_space=pltpu.SMEM)
VMEM_ALL = 60 * 1024 * 1024
VMEM_MOST = 64600 * 1024


def latent_kernel(tok_hbm, w_hbm, gain_hbm, out_ref, tok_v, w_v, gain_v, sems):
    parts, tile, _ = tok_v.shape
    copies = [pltpu.make_async_copy(w_hbm, w_v, sems.at[parts])]
    for i in range(parts):
        copies.append(pltpu.make_async_copy(tok_hbm.at[pl.ds(i * tile, tile)], tok_v.at[i], sems.at[i]))
    copies.append(pltpu.make_async_copy(gain_hbm, gain_v, sems.at[parts + 1]))
    for copy in copies:
        copy.start()
    copies[0].wait()
    copies[-1].wait()
    for i in range(parts):
        copies[1 + i].wait()
        projected = jnp.dot(tok_v[i], w_v[...], preferred_element_type=jnp.float32)
        inv_rms = lax.rsqrt(jnp.mean(projected * projected, axis=-1, keepdims=True) + epsilon)
        out = projected * inv_rms * gain_v[...]
        out_ref[i * tile : (i + 1) * tile, :] = out.astype(out_ref.dtype)


def latents_of(tokens, w_latent, latent_gain):
    rows, width = tokens.shape
    rank = w_latent.shape[1]
    tile = math.gcd(rows, 256)
    return pl.pallas_call(
        latent_kernel,
        in_specs=[ANY, ANY, ANY],
        out_specs=ON_CHIP,
        out_shape=jax.ShapeDtypeStruct((rows, rank), jnp.bfloat16),
        scratch_shapes=[
            VMEM((rows // tile, tile, width), jnp.bfloat16),
            VMEM((width, rank), jnp.bfloat16),
            VMEM((1, rank), jnp.float32),
            DMA((rows // tile + 2,)),
        ],
        cost_estimate=pl.CostEstimate(
            flops=2 * rows * width * rank, bytes_accessed=2 * rows * width, transcendentals=rows
        ),
        compiler_params=pltpu.CompilerParams(vmem_limit_bytes=VMEM_MOST),
        name="latents",
    )(tokens, w_latent, latent_gain.reshape(1, rank))


def query_kernel(tok_hbm, wa_hbm, wb_hbm, oa_hbm, ob_hbm, tok_v, w_v, o_v, tok_sem, w_sem, o_sem):
    m, tile, _ = tok_v.shape
    tiles = w_v.shape[0] // 2
    step = w_v.shape[2]
    core = lax.rem(lax.axis_index("tp"), 2)
    toks = [
        pltpu.make_async_copy(tok_hbm.at[i, core], tok_v.at[i], tok_sem.at[i]) for i in range(m)
    ]
    loads = [
        pltpu.make_async_copy(
            w_hbm.at[:, pl.ds(n * step, step)], w_v.at[u * tiles + n], w_sem.at[u * tiles + n]
        )
        for u, w_hbm in enumerate((wa_hbm, wb_hbm))
        for n in range(tiles)
    ]
    stores = [
        pltpu.make_async_copy(
            o_v.at[u * tiles + n], o_hbm.at[:, pl.ds(n * step, step)], o_sem.at[u * tiles + n]
        )
        for u, o_hbm in enumerate((oa_hbm, ob_hbm))
        for n in range(tiles)
    ]
    for copy in toks + loads[:2]:
        copy.start()
    for n in range(2 * tiles):
        if n + 2 < 2 * tiles:
            loads[n + 2].start()
        loads[n].wait()
        for i in range(m):
            if n == 0:
                toks[i].wait()
            out = jnp.dot(tok_v[i], w_v[n], preferred_element_type=jnp.float32)
            o_v[n, i * tile : (i + 1) * tile, :] = out.astype(o_v.dtype)
        stores[n].start()
    for copy in stores:
        copy.wait()


def queries_of(tokens4, wq_a, wq_b):
    m, _, tile, width = tokens4.shape
    cols = wq_a.shape[1]
    step = math.gcd(cols, 512)
    tiles = cols // step
    shape = jax.ShapeDtypeStruct((m * tile, cols), jnp.bfloat16)
    return pl.pallas_call(
        query_kernel,
        in_specs=[ANY, ANY, ANY],
        out_specs=[ANY, ANY],
        scratch_shapes=[
            VMEM((m, tile, width), jnp.bfloat16),
            VMEM((2 * tiles, width, step), jnp.bfloat16),
            VMEM((2 * tiles, m * tile, step), jnp.bfloat16),
            DMA((m,)),
            DMA((2 * tiles,)),
            DMA((2 * tiles,)),
        ],
        out_shape=[shape, shape],
        cost_estimate=pl.CostEstimate(
            flops=4 * m * tile * width * cols,
            bytes_accessed=4 * width * cols,
            transcendentals=0,
        ),
        compiler_params=pltpu.CompilerParams(vmem_limit_bytes=VMEM_ALL),
        name="queries",
    )(tokens4, wq_a, wq_b)


def pick_kernel(asked_ref, lat_ref, out_ref):
    per_device = lat_ref.shape[0]
    owners, _, count = asked_ref.shape
    first = lax.axis_index("kv") * per_device
    core = lax.rem(lax.axis_index("tp"), 2)
    for i in range(owners):
        for j in range(count):
            block = jnp.clip(asked_ref[i, 0, j] - first, 0, per_device - 1)
            out_ref[i, j] = lat_ref[block, core]


def pick_halves(asked, latent4):
    _, _, half, rank = latent4.shape
    owners, _, count = asked.shape
    return pl.pallas_call(
        pick_kernel,
        in_specs=[SCALARS, ON_CHIP],
        out_specs=ON_CHIP,
        out_shape=jax.ShapeDtypeStruct((owners, count, half, rank), latent4.dtype),
        compiler_params=pltpu.CompilerParams(vmem_limit_bytes=VMEM_MOST),
        name="pick",
    )(asked, latent4)


def project_kernel(ho_hbm, wa_hbm, wb_hbm, out_hbm, ho_v, w_v, out_v, sems, w_sem, out_sem):
    tiles, _, _, step = w_v.shape
    begin = wa_hbm.shape[1] - tiles * step
    hos = [pltpu.make_async_copy(ho_hbm.at[u], ho_v.at[u], sems.at[u]) for u in range(2)]
    for copy in hos:
        copy.start()
    finish_project(begin, ho_v, wa_hbm, wb_hbm, out_hbm, w_v, out_v, w_sem, out_sem, hos)


def finish_project(begin, ho_v, wa_hbm, wb_hbm, out_hbm, w_v, out_v, w_sem, out_sem, hos):
    weights = project_loads(begin, wa_hbm, wb_hbm, w_v, w_sem)
    for copy in weights:
        copy.start()
    for copy in hos:
        copy.wait()
    project_tiles(weights, ho_v, out_hbm, w_v, out_v, out_sem)


def project_loads(begin, wa_hbm, wb_hbm, w_v, w_sem):
    tiles, _, _, step = w_v.shape
    return [
        pltpu.make_async_copy(w_hbm.at[:, pl.ds(begin + n * step, step)], w_v.at[n, u], w_sem.at[n, u])
        for n in range(tiles)
        for u, w_hbm in enumerate((wa_hbm, wb_hbm))
    ]


def project_tiles(weights, ho_v, out_hbm, w_v, out_v, out_sem):
    tiles, _, step = out_v.shape
    stores = []
    for n in range(tiles):
        weights[2 * n].wait()
        weights[2 * n + 1].wait()
        total = jnp.dot(ho_v[0], w_v[n, 0], preferred_element_type=jnp.float32)
        total = total + jnp.dot(ho_v[1], w_v[n, 1], preferred_element_type=jnp.float32)
        out_v[n] = total.astype(out_v.dtype)
        store = pltpu.make_async_copy(out_v.at[n], out_hbm.at[:, pl.ds(n * step, step)], out_sem.at[n])
        store.start()
        stores.append(store)
    for store in stores:
        store.wait()


def project(ho, wo_a, wo_b, width):
    _, rows, cols = ho.shape
    step = math.gcd(width, 512)
    tiles = width // step
    return pl.pallas_call(
        project_kernel,
        in_specs=[ANY] * 3,
        out_specs=ANY,
        scratch_shapes=[
            VMEM((2, rows, cols), jnp.bfloat16),
            VMEM((tiles, 2, cols, step), jnp.bfloat16),
            VMEM((tiles, rows, step), jnp.bfloat16),
            DMA((2,)),
            DMA((tiles, 2)),
            DMA((tiles,)),
        ],
        out_shape=jax.ShapeDtypeStruct((rows, width), jnp.bfloat16),
        cost_estimate=pl.CostEstimate(
            flops=4 * rows * cols * width, bytes_accessed=4 * cols * width, transcendentals=0
        ),
        compiler_params=pltpu.CompilerParams(vmem_limit_bytes=VMEM_ALL),
        name="project",
    )(ho, wo_a, wo_b)


def finish_kernel(own_ref, *refs):
    pieces, (out_hbm, out_v, sems) = refs[:-3], refs[-3:]
    halves, _, part = out_v.shape
    stores = []
    for h in range(halves):
        total = own_ref[:, h * part : (h + 1) * part].astype(jnp.float32)
        for piece in pieces[h::halves]:
            total = total + piece[...].astype(jnp.float32)
        out_v[h] = total.astype(out_v.dtype)
        stores.append(
            pltpu.make_async_copy(out_v.at[h], out_hbm.at[:, pl.ds(h * part, part)], sems.at[h])
        )
        stores[h].start()
    for copy in stores:
        copy.wait()


def finish(own, pieces):
    rows, width = own.shape
    part = width // 2
    return pl.pallas_call(
        finish_kernel,
        in_specs=[ON_CHIP] * (1 + len(pieces)),
        out_specs=ANY,
        out_shape=jax.ShapeDtypeStruct((rows, width), own.dtype),
        scratch_shapes=[VMEM((2, rows, part), own.dtype), DMA((2,))],
        compiler_params=pltpu.CompilerParams(vmem_limit_bytes=12 << 20),
        name="finish",
    )(own, *pieces)


def attend_kernel(
    scale,
    ahead,
    named_hbm,
    qa_hbm,
    qb_hbm,
    own_hbm,
    r1_hbm,
    r2_hbm,
    wa_hbm,
    wb_hbm,
    out_hbm,
    ho_hbm,
    lse_hbm,
    named_ref,
    q_v,
    key_v,
    val_v,
    w_v,
    out_v,
    s0_ref,
    s1_ref,
    p0_ref,
    p1_ref,
    bl_ref,
    ho_ref,
    lse_ref,
    sems,
    w_sem,
    out_sem,
    ho_sem,
):
    _, count, blk_len, cols = q_v.shape
    key_len, rank = key_v.shape
    heads = cols // rank
    own_len = own_hbm.shape[0]
    rem_len = r1_hbm.shape[0]
    half = blk_len // 2
    own_blocks = own_len // blk_len
    slots = rem_len // half
    lanes = bl_ref.shape[2]
    unit = heads * blk_len
    exp_scale = scale * math.log2(math.e)
    tp = lax.axis_index("tp")
    chip = lax.rem(tp // 2 + ahead, qa_hbm.shape[0])
    first = (chip * 2 + lax.rem(tp, 2)) * count
    naming = pltpu.make_async_copy(named_hbm, named_ref, sems.at[5])
    parts = []
    base = 0
    for i, hbm in enumerate((own_hbm, r1_hbm, r2_hbm)):
        n = hbm.shape[0]
        parts.append((pltpu.make_async_copy(hbm, key_v.at[pl.ds(base, n)], sems.at[2 + i]), base, n))
        base += n
    qs = [
        pltpu.make_async_copy(q_hbm.at[chip], q_v.at[u], sems.at[u])
        for u, q_hbm in enumerate((qa_hbm, qb_hbm))
    ]
    weights = project_loads(0, wa_hbm, wb_hbm, w_v, w_sem)
    for copy in [naming, qs[0], parts[0][0], parts[1][0], parts[2][0], qs[1]]:
        copy.start()

    naming.wait()

    def own_bias(b, _):
        k_off = lax.broadcasted_iota(jnp.int32, (blk_len, lanes), 0)
        q_off = lax.broadcasted_iota(jnp.int32, (blk_len, lanes), 1) % blk_len
        here = first + b
        for j in range(own_blocks):
            keep = k_off + (j - here) * blk_len <= q_off
            bl_ref[b, j * blk_len : (j + 1) * blk_len, :] = jnp.where(keep, named_ref[here, j], NEG)
        return 0

    lax.fori_loop(0, count, own_bias, 0)
    chunk = math.gcd(math.gcd(own_len, rem_len), 256)
    for copy in [part[0] for part in parts] + qs:
        copy.wait()
    for copy in weights:
        copy.start()
    for k in range(0, key_len, chunk):
        val_v[:, k : k + chunk] = key_v[k : k + chunk, :].T

    def scores(b, u, s_ref):
        here = first + b
        q = jnp.concatenate(
            [q_v[u, b, :, h * rank : (h + 1) * rank] for h in range(heads)], axis=0
        )
        peak = jnp.full((8, unit), NEG, jnp.float32)
        for at in range(0, key_len, chunk):
            s = lax.dot_general(
                key_v[at : at + chunk, :], q, (((1,), (1,)), ((), ())), preferred_element_type=jnp.float32
            )
            for k in range(0, chunk, half):
                col = at + k
                row = s[k : k + half]
                if col < own_len:
                    add = bl_ref[b, col : col + half, :]
                    row = row + jnp.concatenate([add] * (unit // lanes), axis=1)
                else:
                    row = row + named_ref[here, own_blocks + (col - own_len) // half % slots]
                s_ref[col : col + half, :] = row
                for r in range(0, half, 8):
                    peak = jnp.maximum(peak, row[r : r + 8])
        return jnp.max(peak, axis=0, keepdims=True)

    def weigh(b, u, s_ref, p_ref, peak):
        mass = jnp.zeros((8, unit), jnp.float32)
        for k in range(0, key_len, half):
            raised = jnp.exp2((s_ref[k : k + half, :] - peak) * exp_scale)
            p_ref[k : k + half, :] = raised.astype(p_ref.dtype)
            for r in range(0, half, 8):
                mass = mass + raised[r : r + 8]
        mass = jnp.sum(mass, axis=0, keepdims=True)
        lse_ref[b, u : u + 1, :] = peak * scale + jnp.log(mass)
        return 1.0 / mass

    def gather(b, u, p_ref, inverse):
        out = jnp.dot(val_v[...], p_ref[...], preferred_element_type=jnp.float32)
        out = (out * inverse).astype(ho_ref.dtype).T
        at = pl.multiple_of(b * blk_len, blk_len)
        for h in range(heads):
            ho_ref[u, pl.ds(at, blk_len), h * rank : (h + 1) * rank] = out[h * blk_len : (h + 1) * blk_len]

    def block(b, carry):
        peak0, inverse1 = carry
        peak1 = scores(b, 1, s1_ref)
        inverse0 = weigh(b, 0, s0_ref, p0_ref, peak0)
        gather(jnp.maximum(b - 1, 0), 1, p1_ref, inverse1)
        after = scores(jnp.minimum(b + 1, count - 1), 0, s0_ref)
        inverse1 = weigh(b, 1, s1_ref, p1_ref, peak1)
        gather(b, 0, p0_ref, inverse0)
        return after, inverse1

    p1_ref[...] = jnp.zeros_like(p1_ref)
    start = (scores(0, 0, s0_ref), jnp.ones((1, unit), jnp.float32))
    _, inverse1 = lax.fori_loop(0, count, block, start)
    gather(count - 1, 1, p1_ref, inverse1)
    keeps = [
        pltpu.make_async_copy(ho_ref, ho_hbm, ho_sem.at[0]),
        pltpu.make_async_copy(lse_ref, lse_hbm, ho_sem.at[1]),
    ]
    for copy in keeps:
        copy.start()
    project_tiles(weights, ho_ref, out_hbm, w_v, out_v, out_sem)
    for copy in keeps:
        copy.wait()


def attend(named, qa, qb, latent, r1, r2, wo_a, wo_b, width, ahead, scale):
    _, count, blk_len, cols = qa.shape
    own_len, rank = latent.shape
    heads = cols // rank
    key_len = own_len + 2 * r1.shape[0]
    step = math.gcd(width, 512)
    tiles = width // step
    unit = heads * blk_len
    return pl.pallas_call(
        functools.partial(attend_kernel, scale, ahead),
        in_specs=[ANY] * 8,
        out_specs=[ANY] * 3,
        scratch_shapes=[
                pltpu.SMEM(named.shape, jnp.float32),
                VMEM((2, count, blk_len, cols), jnp.bfloat16),
                VMEM((key_len, rank), jnp.bfloat16),
                VMEM((rank, key_len), jnp.bfloat16),
                VMEM((tiles, 2, cols, step), jnp.bfloat16),
                VMEM((tiles, count * blk_len, step), jnp.bfloat16),
                VMEM((key_len, unit), jnp.float32),
                VMEM((key_len, unit), jnp.float32),
                VMEM((key_len, unit), jnp.bfloat16),
                VMEM((key_len, unit), jnp.bfloat16),
                VMEM((count, own_len, 2 * blk_len), jnp.float32),
                VMEM((2, count * blk_len, cols), jnp.bfloat16),
                VMEM((count, 2, unit), jnp.float32),
                DMA((6,)),
                DMA((tiles, 2)),
                DMA((tiles,)),
                DMA((2,)),
        ],
        out_shape=[
            jax.ShapeDtypeStruct((count * blk_len, width), jnp.bfloat16),
            jax.ShapeDtypeStruct((2, count * blk_len, cols), jnp.bfloat16),
            jax.ShapeDtypeStruct((count, 2, unit), jnp.float32),
        ],
        cost_estimate=pl.CostEstimate(
            flops=8 * count * unit * key_len * rank + 4 * count * blk_len * cols * width,
            bytes_accessed=2 * key_len * rank + 4 * cols * width,
            transcendentals=2 * count * unit * key_len,
        ),
        compiler_params=pltpu.CompilerParams(vmem_limit_bytes=VMEM_ALL),
        name="attend",
    )(named, qa, qb, latent, r1, r2, wo_a, wo_b)


def layer(tokens, w_query, w_latent, latent_gain, w_output, chosen):
    tok_rows, width = tokens.shape
    rank = w_latent.shape[1]
    heads = w_query.shape[1] // rank
    per_device, picks = chosen.shape
    blk_len = tok_rows // per_device
    half = blk_len // 2
    devices = lax.axis_size("kv")
    n_tp = lax.axis_size("tp")
    m = n_tp // 2
    tile_rows = tok_rows // n_tp
    tile_blocks = tile_rows // blk_len
    mine = lax.axis_index("kv")
    tp = lax.axis_index("tp")
    chip, core = tp // 2, tp % 2
    swap = [(i, i ^ 1) for i in range(n_tp)]

    wq_other = lax.ppermute(w_query, "tp", swap)

    flat = chosen.reshape(1, per_device * picks)
    first_id = (jnp.arange(devices, dtype=jnp.int32) * per_device)[:, None]
    of_owner = (flat >= first_id) & (flat < first_id + per_device)
    low = jnp.min(jnp.where(of_owner, flat, devices * per_device), axis=1)
    high = jnp.max(jnp.where(of_owner, flat, -1), axis=1)
    request = jnp.stack([low, high], axis=1)[:, None, :]
    asked = lax.all_to_all(request, "kv", split_axis=0, concat_axis=0, tiled=True)

    latent = latents_of(tokens, w_latent, latent_gain)
    held, latent = lax.optimization_barrier((w_output, latent))
    wo_other = lax.ppermute(held, "tp", swap)
    tokens4 = tokens.reshape(m, 2, tile_rows, width)

    reply = pick_halves(asked, latent.reshape(per_device, 2, half, rank))
    fetched = lax.all_to_all(
        reply, "kv", split_axis=0, concat_axis=0, tiled=True
    )
    r1 = fetched.reshape(devices * CAP * half, rank)
    r2 = lax.ppermute(r1, "tp", swap)
    qa, qb = queries_of(tokens4, w_query, wq_other)

    earlier = jnp.arange(devices, dtype=jnp.int32) < mine
    slots = jnp.stack(
        [jnp.where(earlier, low, -2), jnp.where(earlier & (high > low), high, -2)], axis=1
    ).reshape(devices * CAP)
    own_ids = mine * per_device + jnp.arange(per_device, dtype=jnp.int32)
    key_ids = jnp.concatenate([own_ids, slots])
    named = jnp.any(chosen[:, :, None] == key_ids[None, None, :], axis=1)
    named = jnp.where(named, 0.0, NEG).astype(jnp.float32)

    qa4 = qa.reshape(m, tile_blocks, blk_len, heads * rank)
    qb4 = qb.reshape(m, tile_blocks, blk_len, heads * rank)
    scale = rank ** (-0.5)

    def work(k, cols):
        out, ho, lse = attend(named, qa4, qb4, latent, r1, r2, w_output, wo_other, cols, k, scale)
        return out, ho, lse.reshape(tile_blocks, 2, heads, blk_len)

    lse_tiles = [None] * m
    arrived = []
    part = width // 2
    for k in range(1, m):
        to_chip = [(i, (i + 2 * k) % n_tp) for i in range(n_tp)]
        out0, ho, lse_tiles[k] = work(k, part)
        piece0 = lax.ppermute(out0, "tp", to_chip)
        out1 = project(ho, w_output, wo_other, width - part)
        piece1 = lax.ppermute(out1, "tp", to_chip)
        arrived.append([piece0, piece1])
    total, _, lse_tiles[0] = work(0, width)
    attended = finish(total, sum(arrived, []))

    lse = jnp.stack(lse_tiles)
    lse = lax.dynamic_slice_in_dim(jnp.concatenate([lse, lse], axis=0), (m - chip) % m, m, 0)
    theirs = lax.ppermute(lse[:, :, 1], "tp", swap)
    ours = lse[:, :, 0]
    log_total = jnp.where(
        core == 0, jnp.stack([ours, theirs], axis=1), jnp.stack([theirs, ours], axis=1)
    )
    log_total = jnp.swapaxes(log_total, 3, 4).reshape(tok_rows, heads)
    return (attended, log_total)


def solution(mesh):
    placed = (P("kv", None), P(None, "tp"), P(), P(), P("tp", None), P("kv", None))
    return jax.shard_map(
        layer,
        mesh=mesh,
        in_specs=placed,
        out_specs=(P(("kv", "tp"), None), P("kv", "tp")),
        check_vma=False,
    )
```

```python
import functools
import math

import jax
import jax.numpy as jnp
from jax import lax
from jax.experimental import pallas as pl
from jax.experimental.pallas import tpu as pltpu
from jax.sharding import PartitionSpec as P


CAP = 2
NEG = -1e30
epsilon = 1e-06
VMEM = pltpu.VMEM
DMA = pltpu.SemaphoreType.DMA
ANY = pl.BlockSpec(memory_space=pltpu.HBM)
ON_CHIP = pl.BlockSpec(memory_space=VMEM)
SCALARS = pl.BlockSpec(memory_space=pltpu.SMEM)
VMEM_ALL = 60 * 1024 * 1024
VMEM_PART = 52 << 20


def latent_kernel(tok_ref, w_ref, gain_ref, out_ref):
    tile = math.gcd(tok_ref.shape[0], 256)
    for at in range(0, tok_ref.shape[0], tile):
        projected = jnp.dot(tok_ref[at : at + tile, :], w_ref[...], preferred_element_type=jnp.float32)
        inv_rms = lax.rsqrt(jnp.mean(projected * projected, axis=-1, keepdims=True) + epsilon)
        out = projected * inv_rms * gain_ref[...]
        out_ref[at : at + tile, :] = out.astype(out_ref.dtype)


def latents_of(tokens, w_latent, latent_gain):
    rows, width = tokens.shape
    rank = w_latent.shape[1]
    return pl.pallas_call(
        latent_kernel,
        in_specs=[ON_CHIP] * 3,
        out_specs=ON_CHIP,
        out_shape=jax.ShapeDtypeStruct((rows, rank), jnp.bfloat16),
        cost_estimate=pl.CostEstimate(
            flops=2 * rows * width * rank, bytes_accessed=2 * rows * width, transcendentals=rows
        ),
        compiler_params=pltpu.CompilerParams(vmem_limit_bytes=12 << 20),
        name="latents",
    )(tokens, w_latent, latent_gain.reshape(1, rank))


def query_kernel(tok_hbm, w_hbm, keep_hbm, give_hbm, tok_v, w_v, o_v, tok_sem, w_sem, o_sem):
    _, m, tile, _ = tok_v.shape
    tiles, _, step = w_v.shape
    core = lax.rem(lax.axis_index("tp"), 2)
    toks = [
        pltpu.make_async_copy(tok_hbm.at[i, lax.rem(core + 1 - side, 2)], tok_v.at[side, i], tok_sem.at[side, i])
        for side in range(2)
        for i in range(m)
    ]
    loads = [
        pltpu.make_async_copy(w_hbm.at[:, pl.ds(n * step, step)], w_v.at[n], w_sem.at[n])
        for n in range(tiles)
    ]
    for copy in toks[:m] + loads + toks[m:]:
        copy.start()
    stores = []
    for side, o_hbm in enumerate((give_hbm, keep_hbm)):
        for copy in toks[side * m : side * m + m]:
            copy.wait()
        for n in range(tiles):
            if side == 0:
                loads[n].wait()
            for i in range(m):
                out = jnp.dot(tok_v[side, i], w_v[n], preferred_element_type=jnp.float32)
                o_v[side, n, i * tile : (i + 1) * tile, :] = out.astype(o_v.dtype)
            store = pltpu.make_async_copy(
                o_v.at[side, n], o_hbm.at[:, pl.ds(n * step, step)], o_sem.at[side, n]
            )
            store.start()
            stores.append(store)
    for copy in stores:
        copy.wait()


def queries_of(tokens4, w_query):
    m, _, tile, width = tokens4.shape
    cols = w_query.shape[1]
    step = math.gcd(cols, 512)
    tiles = cols // step
    shape = jax.ShapeDtypeStruct((m * tile, cols), jnp.bfloat16)
    return pl.pallas_call(
        query_kernel,
        in_specs=[ANY, ANY],
        out_specs=[ANY, ANY],
        scratch_shapes=[
            VMEM((2, m, tile, width), jnp.bfloat16),
            VMEM((tiles, width, step), jnp.bfloat16),
            VMEM((2, tiles, m * tile, step), jnp.bfloat16),
            DMA((2, m)),
            DMA((tiles,)),
            DMA((2, tiles)),
        ],
        out_shape=[shape, shape],
        cost_estimate=pl.CostEstimate(
            flops=4 * m * tile * width * cols,
            bytes_accessed=4 * width * cols,
            transcendentals=0,
        ),
        compiler_params=pltpu.CompilerParams(vmem_limit_bytes=VMEM_ALL),
        name="queries",
    )(tokens4, w_query)


def pick_kernel(asked_ref, lat_ref, out_ref):
    per_device = lat_ref.shape[0]
    owners, _, count = asked_ref.shape
    first = lax.axis_index("kv") * per_device
    core = lax.rem(lax.axis_index("tp"), 2)
    for i in range(owners):
        for j in range(count):
            block = jnp.clip(asked_ref[i, 0, j] - first, 0, per_device - 1)
            out_ref[i, j] = lat_ref[block, core]


def pick_halves(asked, latent4):
    _, _, half, rank = latent4.shape
    owners, _, count = asked.shape
    return pl.pallas_call(
        pick_kernel,
        in_specs=[SCALARS, ON_CHIP],
        out_specs=ON_CHIP,
        out_shape=jax.ShapeDtypeStruct((owners, count, half, rank), latent4.dtype),
        compiler_params=pltpu.CompilerParams(vmem_limit_bytes=4 << 20),
        name="pick",
    )(asked, latent4)


def project_kernel(ho_hbm, wa_hbm, wb_hbm, out_hbm, ho_v, w_v, out_v, sems, w_sem, out_sem):
    tiles, _, _, step = w_v.shape
    begin = wa_hbm.shape[1] - tiles * step
    hos = [pltpu.make_async_copy(ho_hbm.at[u], ho_v.at[u], sems.at[u]) for u in range(2)]
    for copy in hos:
        copy.start()
    finish_project(begin, ho_v, wa_hbm, wb_hbm, out_hbm, w_v, out_v, w_sem, out_sem, hos)


def finish_project(begin, ho_v, wa_hbm, wb_hbm, out_hbm, w_v, out_v, w_sem, out_sem, hos):
    weights = project_loads(begin, wa_hbm, wb_hbm, w_v, w_sem)
    for copy in weights:
        copy.start()
    for copy in hos:
        copy.wait()
    project_tiles(weights, ho_v, out_hbm, w_v, out_v, out_sem)


def project_loads(begin, wa_hbm, wb_hbm, w_v, w_sem):
    tiles, _, _, step = w_v.shape
    return [
        pltpu.make_async_copy(w_hbm.at[:, pl.ds(begin + n * step, step)], w_v.at[n, u], w_sem.at[n, u])
        for n in range(tiles)
        for u, w_hbm in enumerate((wa_hbm, wb_hbm))
    ]


def project_tiles(weights, ho_v, out_hbm, w_v, out_v, out_sem):
    tiles, _, step = out_v.shape
    stores = []
    for n in range(tiles):
        weights[2 * n].wait()
        weights[2 * n + 1].wait()
        total = jnp.dot(ho_v[0], w_v[n, 0], preferred_element_type=jnp.float32)
        total = total + jnp.dot(ho_v[1], w_v[n, 1], preferred_element_type=jnp.float32)
        out_v[n] = total.astype(out_v.dtype)
        store = pltpu.make_async_copy(out_v.at[n], out_hbm.at[:, pl.ds(n * step, step)], out_sem.at[n])
        store.start()
        stores.append(store)
    for store in stores:
        store.wait()


def project(ho, wo_a, wo_b, width):
    _, rows, cols = ho.shape
    step = math.gcd(width, 512)
    tiles = width // step
    return pl.pallas_call(
        project_kernel,
        in_specs=[ANY] * 3,
        out_specs=ANY,
        scratch_shapes=[
            VMEM((2, rows, cols), jnp.bfloat16),
            VMEM((tiles, 2, cols, step), jnp.bfloat16),
            VMEM((tiles, rows, step), jnp.bfloat16),
            DMA((2,)),
            DMA((tiles, 2)),
            DMA((tiles,)),
        ],
        out_shape=jax.ShapeDtypeStruct((rows, width), jnp.bfloat16),
        cost_estimate=pl.CostEstimate(
            flops=4 * rows * cols * width, bytes_accessed=4 * cols * width, transcendentals=0
        ),
        compiler_params=pltpu.CompilerParams(vmem_limit_bytes=VMEM_PART),
        name="project",
    )(ho, wo_a, wo_b)


def finish_kernel(own_ref, *refs):
    pieces, (out_hbm, out_v, sems) = refs[:-3], refs[-3:]
    halves, _, part = out_v.shape
    stores = []
    for h in range(halves):
        total = own_ref[:, h * part : (h + 1) * part].astype(jnp.float32)
        for piece in pieces[h::halves]:
            total = total + piece[...].astype(jnp.float32)
        out_v[h] = total.astype(out_v.dtype)
        stores.append(
            pltpu.make_async_copy(out_v.at[h], out_hbm.at[:, pl.ds(h * part, part)], sems.at[h])
        )
        stores[h].start()
    for copy in stores:
        copy.wait()


def finish(own, pieces):
    rows, width = own.shape
    part = width // 2
    return pl.pallas_call(
        finish_kernel,
        in_specs=[ON_CHIP] * (1 + len(pieces)),
        out_specs=ANY,
        out_shape=jax.ShapeDtypeStruct((rows, width), own.dtype),
        scratch_shapes=[VMEM((2, rows, part), own.dtype), DMA((2,))],
        compiler_params=pltpu.CompilerParams(vmem_limit_bytes=12 << 20),
        name="finish",
    )(own, *pieces)


def attend_kernel(
    scale,
    ahead,
    named_hbm,
    qa_hbm,
    qb_hbm,
    own_hbm,
    r1_hbm,
    r2_hbm,
    wa_hbm,
    wb_hbm,
    out_hbm,
    ho_hbm,
    lse_hbm,
    named_ref,
    q_v,
    key_v,
    val_v,
    w_v,
    out_v,
    s0_ref,
    s1_ref,
    p0_ref,
    p1_ref,
    bl_ref,
    ho_ref,
    lse_ref,
    sems,
    w_sem,
    out_sem,
    ho_sem,
):
    _, count, blk_len, cols = q_v.shape
    key_len, rank = key_v.shape
    heads = cols // rank
    own_len = own_hbm.shape[0]
    rem_len = r1_hbm.shape[0]
    half = blk_len // 2
    own_blocks = own_len // blk_len
    slots = rem_len // half
    lanes = bl_ref.shape[2]
    unit = heads * blk_len
    exp_scale = scale * math.log2(math.e)
    tp = lax.axis_index("tp")
    chip = lax.rem(tp // 2 + ahead, qa_hbm.shape[0])
    first = (chip * 2 + lax.rem(tp, 2)) * count
    naming = pltpu.make_async_copy(named_hbm, named_ref, sems.at[5])
    parts = []
    base = 0
    for i, hbm in enumerate((own_hbm, r1_hbm, r2_hbm)):
        n = hbm.shape[0]
        parts.append((pltpu.make_async_copy(hbm, key_v.at[pl.ds(base, n)], sems.at[2 + i]), base, n))
        base += n
    qs = [
        pltpu.make_async_copy(q_hbm.at[chip], q_v.at[u], sems.at[u])
        for u, q_hbm in enumerate((qa_hbm, qb_hbm))
    ]
    weights = project_loads(0, wa_hbm, wb_hbm, w_v, w_sem)
    for copy in [naming, qs[0], parts[0][0], parts[1][0], parts[2][0], qs[1]]:
        copy.start()

    naming.wait()

    def own_bias(b, _):
        k_off = lax.broadcasted_iota(jnp.int32, (blk_len, lanes), 0)
        q_off = lax.broadcasted_iota(jnp.int32, (blk_len, lanes), 1) % blk_len
        here = first + b
        for j in range(own_blocks):
            keep = k_off + (j - here) * blk_len <= q_off
            bl_ref[b, j * blk_len : (j + 1) * blk_len, :] = jnp.where(keep, named_ref[here, j], NEG)
        return 0

    lax.fori_loop(0, count, own_bias, 0)
    chunk = math.gcd(math.gcd(own_len, rem_len), 256)
    for copy in [part[0] for part in parts] + qs:
        copy.wait()
    for copy in weights:
        copy.start()
    for k in range(0, key_len, chunk):
        val_v[:, k : k + chunk] = key_v[k : k + chunk, :].T

    def queries(b, u):
        return jnp.concatenate(
            [q_v[u, b, :, h * rank : (h + 1) * rank] for h in range(heads)], axis=0
        )

    def scores(at, b, q, s_ref, peak):
        here = first + b
        s = lax.dot_general(
            key_v[at : at + chunk, :], q, (((1,), (1,)), ((), ())), preferred_element_type=jnp.float32
        )
        for k in range(0, chunk, half):
            col = at + k
            row = s[k : k + half]
            if col < own_len:
                add = bl_ref[b, col : col + half, :]
                row = row + jnp.concatenate([add] * (unit // lanes), axis=1)
            else:
                row = row + named_ref[here, own_blocks + (col - own_len) // half % slots]
            s_ref[col : col + half, :] = row
            for r in range(0, half, 8):
                peak = jnp.maximum(peak, row[r : r + 8])
        return peak

    def weigh(at, s_ref, p_ref, peak, mass):
        for k in range(at, at + chunk, half):
            raised = jnp.exp2((s_ref[k : k + half, :] - peak) * exp_scale)
            p_ref[k : k + half, :] = raised.astype(p_ref.dtype)
            for r in range(0, half, 8):
                mass = mass + raised[r : r + 8]
        return mass

    def place(b, u, out, inverse):
        out = (out * inverse).astype(ho_ref.dtype).T
        at = pl.multiple_of(b * blk_len, blk_len)
        for h in range(heads):
            ho_ref[u, pl.ds(at, blk_len), h * rank : (h + 1) * rank] = out[h * blk_len : (h + 1) * blk_len]

    low = jnp.full((8, unit), NEG, jnp.float32)
    top = lambda peak: jnp.max(peak, axis=0, keepdims=True)

    def stage(score, weight, gather):
        b, u, s_ref = score
        q = queries(b, u)
        next_peak = low
        b1, u1, s1, p1, peak = weight
        mass = jnp.zeros((8, unit), jnp.float32)
        b2, u2, p2, inverse = gather
        out = jnp.zeros((rank, unit), jnp.float32)
        for at in range(0, key_len, chunk):
            out = out + jnp.dot(
                val_v[:, at : at + chunk], p2[at : at + chunk, :], preferred_element_type=jnp.float32
            )
            mass = weigh(at, s1, p1, peak, mass)
            next_peak = scores(at, b, q, s_ref, next_peak)
        place(b2, u2, out, inverse)
        mass = jnp.sum(mass, axis=0, keepdims=True)
        lse_ref[b1, u1 : u1 + 1, :] = peak * scale + jnp.log(mass)
        return top(next_peak), 1.0 / mass

    def block(b, carry):
        peak, inverse = carry
        before = jnp.maximum(b - 1, 0)
        after = jnp.minimum(b + 1, count - 1)
        peak, inverse = stage((b, 1, s1_ref), (b, 0, s0_ref, p0_ref, peak), (before, 1, p1_ref, inverse))
        return stage((after, 0, s0_ref), (b, 1, s1_ref, p1_ref, peak), (b, 0, p0_ref, inverse))

    p1_ref[...] = jnp.zeros_like(p1_ref)
    q0 = queries(0, 0)
    peak0 = low
    for at in range(0, key_len, chunk):
        peak0 = scores(at, 0, q0, s0_ref, peak0)
    start = (top(peak0), jnp.ones((1, unit), jnp.float32))
    _, inverse1 = lax.fori_loop(0, count, block, start)
    place(count - 1, 1, jnp.dot(val_v[...], p1_ref[...], preferred_element_type=jnp.float32), inverse1)
    keeps = [
        pltpu.make_async_copy(ho_ref, ho_hbm, ho_sem.at[0]),
        pltpu.make_async_copy(lse_ref, lse_hbm, ho_sem.at[1]),
    ]
    for copy in keeps:
        copy.start()
    project_tiles(weights, ho_ref, out_hbm, w_v, out_v, out_sem)
    for copy in keeps:
        copy.wait()


def attend(named, qa, qb, latent, r1, r2, wo_a, wo_b, width, ahead, scale):
    _, count, blk_len, cols = qa.shape
    own_len, rank = latent.shape
    heads = cols // rank
    key_len = own_len + 2 * r1.shape[0]
    step = math.gcd(width, 512)
    tiles = width // step
    unit = heads * blk_len
    return pl.pallas_call(
        functools.partial(attend_kernel, scale, ahead),
        in_specs=[ANY] * 8,
        out_specs=[ANY] * 3,
        scratch_shapes=[
                pltpu.SMEM(named.shape, jnp.float32),
                VMEM((2, count, blk_len, cols), jnp.bfloat16),
                VMEM((key_len, rank), jnp.bfloat16),
                VMEM((rank, key_len), jnp.bfloat16),
                VMEM((tiles, 2, cols, step), jnp.bfloat16),
                VMEM((tiles, count * blk_len, step), jnp.bfloat16),
                VMEM((key_len, unit), jnp.float32),
                VMEM((key_len, unit), jnp.float32),
                VMEM((key_len, unit), jnp.bfloat16),
                VMEM((key_len, unit), jnp.bfloat16),
                VMEM((count, own_len, 2 * blk_len), jnp.float32),
                VMEM((2, count * blk_len, cols), jnp.bfloat16),
                VMEM((count, 2, unit), jnp.float32),
                DMA((6,)),
                DMA((tiles, 2)),
                DMA((tiles,)),
                DMA((2,)),
        ],
        out_shape=[
            jax.ShapeDtypeStruct((count * blk_len, width), jnp.bfloat16),
            jax.ShapeDtypeStruct((2, count * blk_len, cols), jnp.bfloat16),
            jax.ShapeDtypeStruct((count, 2, unit), jnp.float32),
        ],
        cost_estimate=pl.CostEstimate(
            flops=8 * count * unit * key_len * rank + 4 * count * blk_len * cols * width,
            bytes_accessed=2 * key_len * rank + 4 * cols * width,
            transcendentals=2 * count * unit * key_len,
        ),
        compiler_params=pltpu.CompilerParams(vmem_limit_bytes=VMEM_PART),
        name="attend",
    )(named, qa, qb, latent, r1, r2, wo_a, wo_b)


def layer(tokens, w_query, w_latent, latent_gain, w_output, chosen):
    tok_rows, width = tokens.shape
    rank = w_latent.shape[1]
    heads = w_query.shape[1] // rank
    per_device, picks = chosen.shape
    blk_len = tok_rows // per_device
    half = blk_len // 2
    devices = lax.axis_size("kv")
    n_tp = lax.axis_size("tp")
    m = n_tp // 2
    tile_rows = tok_rows // n_tp
    tile_blocks = tile_rows // blk_len
    mine = lax.axis_index("kv")
    tp = lax.axis_index("tp")
    chip, core = tp // 2, tp % 2
    swap = [(i, i ^ 1) for i in range(n_tp)]


    flat = chosen.reshape(1, per_device * picks)
    first_id = (jnp.arange(devices, dtype=jnp.int32) * per_device)[:, None]
    of_owner = (flat >= first_id) & (flat < first_id + per_device)
    low = jnp.min(jnp.where(of_owner, flat, devices * per_device), axis=1)
    high = jnp.max(jnp.where(of_owner, flat, -1), axis=1)
    request = jnp.stack([low, high], axis=1)[:, None, :]
    asked = lax.all_to_all(request, "kv", split_axis=0, concat_axis=0, tiled=True)

    latent = latents_of(tokens, w_latent, latent_gain)
    held, latent = lax.optimization_barrier((w_output, latent))
    wo_other = lax.ppermute(held, "tp", swap)
    tokens4 = tokens.reshape(m, 2, tile_rows, width)

    reply = pick_halves(asked, latent.reshape(per_device, 2, half, rank))
    fetched = lax.all_to_all(
        reply, "kv", split_axis=0, concat_axis=0, tiled=True
    )
    r1 = fetched.reshape(devices * CAP * half, rank)
    r2 = lax.ppermute(r1, "tp", swap)
    qa, give = queries_of(tokens4, w_query)
    qb = lax.ppermute(give, "tp", swap)

    earlier = jnp.arange(devices, dtype=jnp.int32) < mine
    slots = jnp.stack(
        [jnp.where(earlier, low, -2), jnp.where(earlier & (high > low), high, -2)], axis=1
    ).reshape(devices * CAP)
    own_ids = mine * per_device + jnp.arange(per_device, dtype=jnp.int32)
    key_ids = jnp.concatenate([own_ids, slots])
    named = jnp.any(chosen[:, :, None] == key_ids[None, None, :], axis=1)
    named = jnp.where(named, 0.0, NEG).astype(jnp.float32)

    qa4 = qa.reshape(m, tile_blocks, blk_len, heads * rank)
    qb4 = qb.reshape(m, tile_blocks, blk_len, heads * rank)
    scale = rank ** (-0.5)

    def work(k, cols):
        out, ho, lse = attend(named, qa4, qb4, latent, r1, r2, w_output, wo_other, cols, k, scale)
        theirs = lax.ppermute(lse[:, 1], "tp", swap)
        return out, ho, (lse[:, 0], theirs)

    lse_tiles = [None] * m
    arrived = []
    part = width // 2
    for k in range(1, m):
        to_chip = [(i, (i + 2 * k) % n_tp) for i in range(n_tp)]
        out0, ho, lse_tiles[k] = work(k, part)
        piece0 = lax.ppermute(out0, "tp", to_chip)
        out1 = project(ho, w_output, wo_other, width - part)
        piece1 = lax.ppermute(out1, "tp", to_chip)
        arrived.append([piece0, piece1])
    total, _, lse_tiles[0] = work(0, width)
    attended = finish(total, sum(arrived, []))

    tiles = []
    for c in range(m):
        for side in range(2):
            at = [lax.rem(c - chip + m, m) == k for k in range(m)]
            ours, theirs = (sum(jnp.where(at[k], lse_tiles[k][i], 0.0) for k in range(m)) for i in range(2))
            tiles.append(jnp.where(core == side, ours, theirs))
    log_total = jnp.stack(tiles).reshape(n_tp * tile_blocks, heads, blk_len)
    log_total = jnp.swapaxes(log_total, 1, 2).reshape(tok_rows, heads)
    return (attended, log_total)


def solution(mesh):
    placed = (P("kv", None), P(None, "tp"), P(), P(), P("tp", None), P("kv", None))
    return jax.shard_map(
        layer,
        mesh=mesh,
        in_specs=placed,
        out_specs=(P(("kv", "tp"), None), P("kv", "tp")),
        check_vma=False,
    )
```

```python
import functools
import math

import jax
import jax.numpy as jnp
from jax import lax
from jax.experimental import pallas as pl
from jax.experimental.pallas import tpu as pltpu
from jax.sharding import PartitionSpec as P


CAP = 2
NEG = -1e30
epsilon = 1e-06
VMEM = pltpu.VMEM
DMA = pltpu.SemaphoreType.DMA
ANY = pl.BlockSpec(memory_space=pltpu.HBM)
ON_CHIP = pl.BlockSpec(memory_space=VMEM)
SCALARS = pl.BlockSpec(memory_space=pltpu.SMEM)
VMEM_ALL = 60 * 1024 * 1024
VMEM_PART = 52 << 20


def latent_kernel(tok_ref, w_ref, gain_ref, out_ref):
    tile = math.gcd(tok_ref.shape[0], 256)
    for at in range(0, tok_ref.shape[0], tile):
        projected = jnp.dot(tok_ref[at : at + tile, :], w_ref[...], preferred_element_type=jnp.float32)
        inv_rms = lax.rsqrt(jnp.mean(projected * projected, axis=-1, keepdims=True) + epsilon)
        out = projected * inv_rms * gain_ref[...]
        out_ref[at : at + tile, :] = out.astype(out_ref.dtype)


def latents_of(tokens, w_latent, latent_gain):
    rows, width = tokens.shape
    rank = w_latent.shape[1]
    return pl.pallas_call(
        latent_kernel,
        in_specs=[ON_CHIP] * 3,
        out_specs=ON_CHIP,
        out_shape=jax.ShapeDtypeStruct((rows, rank), jnp.bfloat16),
        cost_estimate=pl.CostEstimate(
            flops=2 * rows * width * rank, bytes_accessed=2 * rows * width, transcendentals=rows
        ),
        compiler_params=pltpu.CompilerParams(vmem_limit_bytes=12 << 20),
        name="latents",
    )(tokens, w_latent, latent_gain.reshape(1, rank))


def query_kernel(tok_hbm, w_hbm, keep_hbm, give_hbm, tok_v, w_v, o_v, tok_sem, w_sem, o_sem):
    _, m, tile, _ = tok_v.shape
    tiles, _, step = w_v.shape
    core = lax.rem(lax.axis_index("tp"), 2)
    toks = [
        pltpu.make_async_copy(tok_hbm.at[i, lax.rem(core + 1 - side, 2)], tok_v.at[side, i], tok_sem.at[side, i])
        for side in range(2)
        for i in range(m)
    ]
    loads = [
        pltpu.make_async_copy(w_hbm.at[:, pl.ds(n * step, step)], w_v.at[n], w_sem.at[n])
        for n in range(tiles)
    ]
    for copy in toks[:m] + loads + toks[m:]:
        copy.start()
    stores = []
    for side, o_hbm in enumerate((give_hbm, keep_hbm)):
        for copy in toks[side * m : side * m + m]:
            copy.wait()
        for n in range(tiles):
            if side == 0:
                loads[n].wait()
            for i in range(m):
                out = jnp.dot(tok_v[side, i], w_v[n], preferred_element_type=jnp.float32)
                o_v[side, n, i * tile : (i + 1) * tile, :] = out.astype(o_v.dtype)
            store = pltpu.make_async_copy(
                o_v.at[side, n], o_hbm.at[:, pl.ds(n * step, step)], o_sem.at[side, n]
            )
            store.start()
            stores.append(store)
    for copy in stores:
        copy.wait()


def queries_of(tokens4, w_query):
    m, _, tile, width = tokens4.shape
    cols = w_query.shape[1]
    step = math.gcd(cols, 512)
    tiles = cols // step
    shape = jax.ShapeDtypeStruct((m * tile, cols), jnp.bfloat16)
    return pl.pallas_call(
        query_kernel,
        in_specs=[ANY, ANY],
        out_specs=[ANY, ANY],
        scratch_shapes=[
            VMEM((2, m, tile, width), jnp.bfloat16),
            VMEM((tiles, width, step), jnp.bfloat16),
            VMEM((2, tiles, m * tile, step), jnp.bfloat16),
            DMA((2, m)),
            DMA((tiles,)),
            DMA((2, tiles)),
        ],
        out_shape=[shape, shape],
        cost_estimate=pl.CostEstimate(
            flops=4 * m * tile * width * cols,
            bytes_accessed=4 * width * cols,
            transcendentals=0,
        ),
        compiler_params=pltpu.CompilerParams(vmem_limit_bytes=VMEM_ALL),
        name="queries",
    )(tokens4, w_query)


def pick_kernel(asked_ref, lat_ref, out_ref):
    per_device = lat_ref.shape[0]
    owners, _, count = asked_ref.shape
    first = lax.axis_index("kv") * per_device
    core = lax.rem(lax.axis_index("tp"), 2)
    for i in range(owners):
        for j in range(count):
            block = jnp.clip(asked_ref[i, 0, j] - first, 0, per_device - 1)
            out_ref[i, j] = lat_ref[block, core]


def pick_halves(asked, latent4):
    _, _, half, rank = latent4.shape
    owners, _, count = asked.shape
    return pl.pallas_call(
        pick_kernel,
        in_specs=[SCALARS, ON_CHIP],
        out_specs=ON_CHIP,
        out_shape=jax.ShapeDtypeStruct((owners, count, half, rank), latent4.dtype),
        compiler_params=pltpu.CompilerParams(vmem_limit_bytes=4 << 20),
        name="pick",
    )(asked, latent4)


def project_kernel(ho_hbm, wa_hbm, wb_hbm, out_hbm, ho_v, w_v, out_v, sems, w_sem, out_sem):
    tiles, _, _, step = w_v.shape
    begin = wa_hbm.shape[1] - tiles * step
    hos = [pltpu.make_async_copy(ho_hbm.at[u], ho_v.at[u], sems.at[u]) for u in range(2)]
    for copy in hos:
        copy.start()
    finish_project(begin, ho_v, wa_hbm, wb_hbm, out_hbm, w_v, out_v, w_sem, out_sem, hos)


def finish_project(begin, ho_v, wa_hbm, wb_hbm, out_hbm, w_v, out_v, w_sem, out_sem, hos):
    weights = project_loads(begin, wa_hbm, wb_hbm, w_v, w_sem)
    for copy in weights:
        copy.start()
    for copy in hos:
        copy.wait()
    project_tiles(weights, ho_v, out_hbm, w_v, out_v, out_sem)


def project_loads(begin, wa_hbm, wb_hbm, w_v, w_sem):
    tiles, _, _, step = w_v.shape
    return [
        pltpu.make_async_copy(w_hbm.at[:, pl.ds(begin + n * step, step)], w_v.at[n, u], w_sem.at[n, u])
        for n in range(tiles)
        for u, w_hbm in enumerate((wa_hbm, wb_hbm))
    ]


def project_tiles(weights, ho_v, out_hbm, w_v, out_v, out_sem):
    tiles, _, step = out_v.shape
    stores = []
    for n in range(tiles):
        weights[2 * n].wait()
        weights[2 * n + 1].wait()
        total = jnp.dot(ho_v[0], w_v[n, 0], preferred_element_type=jnp.float32)
        total = total + jnp.dot(ho_v[1], w_v[n, 1], preferred_element_type=jnp.float32)
        out_v[n] = total.astype(out_v.dtype)
        store = pltpu.make_async_copy(out_v.at[n], out_hbm.at[:, pl.ds(n * step, step)], out_sem.at[n])
        store.start()
        stores.append(store)
    for store in stores:
        store.wait()


def project(ho, wo_a, wo_b, width):
    _, rows, cols = ho.shape
    step = math.gcd(width, 512)
    tiles = width // step
    return pl.pallas_call(
        project_kernel,
        in_specs=[ANY] * 3,
        out_specs=ANY,
        scratch_shapes=[
            VMEM((2, rows, cols), jnp.bfloat16),
            VMEM((tiles, 2, cols, step), jnp.bfloat16),
            VMEM((tiles, rows, step), jnp.bfloat16),
            DMA((2,)),
            DMA((tiles, 2)),
            DMA((tiles,)),
        ],
        out_shape=jax.ShapeDtypeStruct((rows, width), jnp.bfloat16),
        cost_estimate=pl.CostEstimate(
            flops=4 * rows * cols * width, bytes_accessed=4 * cols * width, transcendentals=0
        ),
        compiler_params=pltpu.CompilerParams(vmem_limit_bytes=VMEM_PART),
        name="project",
    )(ho, wo_a, wo_b)


def finish_kernel(own_ref, *refs):
    pieces, (out_hbm, out_v, sems) = refs[:-3], refs[-3:]
    halves, _, part = out_v.shape
    stores = []
    for h in range(halves):
        total = own_ref[:, h * part : (h + 1) * part].astype(jnp.float32)
        for piece in pieces[h::halves]:
            total = total + piece[...].astype(jnp.float32)
        out_v[h] = total.astype(out_v.dtype)
        stores.append(
            pltpu.make_async_copy(out_v.at[h], out_hbm.at[:, pl.ds(h * part, part)], sems.at[h])
        )
        stores[h].start()
    for copy in stores:
        copy.wait()


def finish(own, pieces):
    rows, width = own.shape
    part = width // 2
    return pl.pallas_call(
        finish_kernel,
        in_specs=[ON_CHIP] * (1 + len(pieces)),
        out_specs=ANY,
        out_shape=jax.ShapeDtypeStruct((rows, width), own.dtype),
        scratch_shapes=[VMEM((2, rows, part), own.dtype), DMA((2,))],
        compiler_params=pltpu.CompilerParams(vmem_limit_bytes=12 << 20),
        name="finish",
    )(own, *pieces)


def attend_kernel(
    scale,
    ahead,
    groups,
    named_hbm,
    qa_hbm,
    qb_hbm,
    own_hbm,
    r1_hbm,
    r2_hbm,
    wa_hbm,
    wb_hbm,
    out_hbm,
    ho_hbm,
    lse_hbm,
    named_ref,
    q_v,
    key_v,
    val_v,
    w_v,
    out_v,
    s0_ref,
    s1_ref,
    p0_ref,
    p1_ref,
    bl_ref,
    ho_ref,
    lse_ref,
    sems,
    w_sem,
    out_sem,
    ho_sem,
):
    _, count, blk_len, cols = q_v.shape
    key_len, rank = key_v.shape
    heads = cols // rank
    own_len = own_hbm.shape[0]
    rem_len = r1_hbm.shape[0]
    half = blk_len // 2
    own_blocks = own_len // blk_len
    slots = rem_len // half
    lanes = bl_ref.shape[2]
    unit = 2 // groups * heads * blk_len
    exp_scale = scale * math.log2(math.e)
    tp = lax.axis_index("tp")
    chip = lax.rem(tp // 2 + ahead, qa_hbm.shape[0])
    first = (chip * 2 + lax.rem(tp, 2)) * count
    naming = pltpu.make_async_copy(named_hbm, named_ref, sems.at[5])
    parts = []
    base = 0
    for i, hbm in enumerate((own_hbm, r1_hbm, r2_hbm)):
        n = hbm.shape[0]
        parts.append((pltpu.make_async_copy(hbm, key_v.at[pl.ds(base, n)], sems.at[2 + i]), base, n))
        base += n
    qs = [
        pltpu.make_async_copy(q_hbm.at[chip], q_v.at[u], sems.at[u])
        for u, q_hbm in enumerate((qa_hbm, qb_hbm))
    ]
    weights = project_loads(0, wa_hbm, wb_hbm, w_v, w_sem)
    for copy in [naming, qs[0], parts[0][0], parts[1][0], parts[2][0], qs[1]]:
        copy.start()

    naming.wait()

    def own_bias(b, _):
        k_off = lax.broadcasted_iota(jnp.int32, (blk_len, lanes), 0)
        q_off = lax.broadcasted_iota(jnp.int32, (blk_len, lanes), 1) % blk_len
        here = first + b
        for j in range(own_blocks):
            keep = k_off + (j - here) * blk_len <= q_off
            bl_ref[b, j * blk_len : (j + 1) * blk_len, :] = jnp.where(keep, named_ref[here, j], NEG)
        return 0

    lax.fori_loop(0, count, own_bias, 0)
    chunk = math.gcd(math.gcd(own_len, rem_len), 256)
    for copy in [part[0] for part in parts] + qs:
        copy.wait()
    for copy in weights:
        copy.start()
    for k in range(0, key_len, chunk):
        val_v[:, k : k + chunk] = key_v[k : k + chunk, :].T

    sides = 2 // groups

    def queries(b, g):
        return jnp.concatenate(
            [
                q_v[u, b, :, h * rank : (h + 1) * rank]
                for u in range(g * sides, (g + 1) * sides)
                for h in range(heads)
            ],
            axis=0,
        )

    def scores(at, b, q, s_ref, peak):
        here = first + b
        s = lax.dot_general(
            key_v[at : at + chunk, :], q, (((1,), (1,)), ((), ())), preferred_element_type=jnp.float32
        )
        for k in range(0, chunk, half):
            col = at + k
            row = s[k : k + half]
            if col < own_len:
                add = bl_ref[b, col : col + half, :]
                row = row + jnp.concatenate([add] * (unit // lanes), axis=1)
            else:
                row = row + named_ref[here, own_blocks + (col - own_len) // half % slots]
            s_ref[col : col + half, :] = row
            for r in range(0, half, 8):
                peak = jnp.maximum(peak, row[r : r + 8])
        return peak

    def weigh(at, s_ref, p_ref, peak, mass):
        for k in range(at, at + chunk, half):
            raised = jnp.exp2((s_ref[k : k + half, :] - peak) * exp_scale)
            p_ref[k : k + half, :] = raised.astype(p_ref.dtype)
            for r in range(0, half, 8):
                mass = mass + raised[r : r + 8]
        return mass

    def place(b, g, out, inverse):
        out = (out * inverse).astype(ho_ref.dtype).T
        for i in range(sides * heads):
            u, h = g * sides + i // heads, i % heads
            ho_ref[u, b * blk_len : (b + 1) * blk_len, h * rank : (h + 1) * rank] = out[
                i * blk_len : (i + 1) * blk_len
            ]

    units = [(b, g) for b in range(count) for g in range(groups)]
    s_refs, p_refs = (s0_ref, s1_ref), (p0_ref, p1_ref)
    peaks, inverses = {}, {}
    for t in range(-1, len(units) + 1):
        score, weight, gather = t + 1 < len(units), 0 <= t < len(units), t >= 1
        if score:
            q = queries(*units[t + 1])
            peak = jnp.full((8, unit), NEG, jnp.float32)
        if weight:
            mass = jnp.zeros((8, unit), jnp.float32)
        if gather:
            out = jnp.zeros((rank, unit), jnp.float32)
        for at in range(0, key_len, chunk):
            if gather:
                out = out + jnp.dot(
                    val_v[:, at : at + chunk],
                    p_refs[(t - 1) % 2][at : at + chunk, :],
                    preferred_element_type=jnp.float32,
                )
            if weight:
                mass = weigh(at, s_refs[t % 2], p_refs[t % 2], peaks[t], mass)
            if score:
                peak = scores(at, units[t + 1][0], q, s_refs[(t + 1) % 2], peak)
        if gather:
            place(*units[t - 1], out, inverses[t - 1])
        if weight:
            b, g = units[t]
            mass = jnp.sum(mass, axis=0, keepdims=True)
            inverses[t] = 1.0 / mass
            total = peaks[t] * scale + jnp.log(mass)
            for i in range(sides):
                part = unit // sides
                lse_ref[b, g * sides + i : g * sides + i + 1, :] = total[:, i * part : (i + 1) * part]
        if score:
            peaks[t + 1] = jnp.max(peak, axis=0, keepdims=True)
    keeps = [
        pltpu.make_async_copy(ho_ref, ho_hbm, ho_sem.at[0]),
        pltpu.make_async_copy(lse_ref, lse_hbm, ho_sem.at[1]),
    ]
    for copy in keeps:
        copy.start()
    project_tiles(weights, ho_ref, out_hbm, w_v, out_v, out_sem)
    for copy in keeps:
        copy.wait()


def attend(named, qa, qb, latent, r1, r2, wo_a, wo_b, width, ahead, scale):
    _, count, blk_len, cols = qa.shape
    own_len, rank = latent.shape
    heads = cols // rank
    key_len = own_len + 2 * r1.shape[0]
    step = math.gcd(width, 1024)
    tiles = width // step
    side = heads * blk_len
    groups = 1 if key_len <= 4096 else 2
    unit = 2 // groups * side
    return pl.pallas_call(
        functools.partial(attend_kernel, scale, ahead, groups),
        in_specs=[ANY] * 8,
        out_specs=[ANY] * 3,
        scratch_shapes=[
                pltpu.SMEM(named.shape, jnp.float32),
                VMEM((2, count, blk_len, cols), jnp.bfloat16),
                VMEM((key_len, rank), jnp.bfloat16),
                VMEM((rank, key_len), jnp.bfloat16),
                VMEM((tiles, 2, cols, step), jnp.bfloat16),
                VMEM((tiles, count * blk_len, step), jnp.bfloat16),
                VMEM((key_len, unit), jnp.float32),
                VMEM((key_len, unit), jnp.float32),
                VMEM((key_len, unit), jnp.bfloat16),
                VMEM((key_len, unit), jnp.bfloat16),
                VMEM((count, own_len, 2 * blk_len), jnp.float32),
                VMEM((2, count * blk_len, cols), jnp.bfloat16),
                VMEM((count, 2, side), jnp.float32),
                DMA((6,)),
                DMA((tiles, 2)),
                DMA((tiles,)),
                DMA((2,)),
        ],
        out_shape=[
            jax.ShapeDtypeStruct((count * blk_len, width), jnp.bfloat16),
            jax.ShapeDtypeStruct((2, count * blk_len, cols), jnp.bfloat16),
            jax.ShapeDtypeStruct((count, 2, side), jnp.float32),
        ],
        cost_estimate=pl.CostEstimate(
            flops=8 * count * side * key_len * rank + 4 * count * blk_len * cols * width,
            bytes_accessed=2 * key_len * rank + 4 * cols * width,
            transcendentals=2 * count * side * key_len,
        ),
        compiler_params=pltpu.CompilerParams(vmem_limit_bytes=VMEM_PART),
        name="attend",
    )(named, qa, qb, latent, r1, r2, wo_a, wo_b)


def layer(tokens, w_query, w_latent, latent_gain, w_output, chosen):
    tok_rows, width = tokens.shape
    rank = w_latent.shape[1]
    heads = w_query.shape[1] // rank
    per_device, picks = chosen.shape
    blk_len = tok_rows // per_device
    half = blk_len // 2
    devices = lax.axis_size("kv")
    n_tp = lax.axis_size("tp")
    m = n_tp // 2
    tile_rows = tok_rows // n_tp
    tile_blocks = tile_rows // blk_len
    mine = lax.axis_index("kv")
    tp = lax.axis_index("tp")
    chip, core = tp // 2, tp % 2
    swap = [(i, i ^ 1) for i in range(n_tp)]


    flat = chosen.reshape(1, per_device * picks)
    first_id = (jnp.arange(devices, dtype=jnp.int32) * per_device)[:, None]
    of_owner = (flat >= first_id) & (flat < first_id + per_device)
    low = jnp.min(jnp.where(of_owner, flat, devices * per_device), axis=1)
    high = jnp.max(jnp.where(of_owner, flat, -1), axis=1)
    request = jnp.stack([low, high], axis=1)[:, None, :]
    asked = lax.all_to_all(request, "kv", split_axis=0, concat_axis=0, tiled=True)

    latent = latents_of(tokens, w_latent, latent_gain)
    held, latent = lax.optimization_barrier((w_output, latent))
    wo_other = lax.ppermute(held, "tp", swap)
    tokens4 = tokens.reshape(m, 2, tile_rows, width)

    reply = pick_halves(asked, latent.reshape(per_device, 2, half, rank))
    fetched = lax.all_to_all(
        reply, "kv", split_axis=0, concat_axis=0, tiled=True
    )
    r1 = fetched.reshape(devices * CAP * half, rank)
    r2 = lax.ppermute(r1, "tp", swap)
    qa, give = queries_of(tokens4, w_query)
    qb = lax.ppermute(give, "tp", swap)

    earlier = jnp.arange(devices, dtype=jnp.int32) < mine
    slots = jnp.stack(
        [jnp.where(earlier, low, -2), jnp.where(earlier & (high > low), high, -2)], axis=1
    ).reshape(devices * CAP)
    own_ids = mine * per_device + jnp.arange(per_device, dtype=jnp.int32)
    key_ids = jnp.concatenate([own_ids, slots])
    named = jnp.any(chosen[:, :, None] == key_ids[None, None, :], axis=1)
    named = jnp.where(named, 0.0, NEG).astype(jnp.float32)

    qa4 = qa.reshape(m, tile_blocks, blk_len, heads * rank)
    qb4 = qb.reshape(m, tile_blocks, blk_len, heads * rank)
    scale = rank ** (-0.5)

    def work(k, cols):
        out, ho, lse = attend(named, qa4, qb4, latent, r1, r2, w_output, wo_other, cols, k, scale)
        theirs = lax.ppermute(lse[:, 1], "tp", swap)
        return out, ho, (lse[:, 0], theirs)

    lse_tiles = [None] * m
    arrived = []
    part = width // 2
    for k in range(1, m):
        to_chip = [(i, (i + 2 * k) % n_tp) for i in range(n_tp)]
        out0, ho, lse_tiles[k] = work(k, part)
        piece0 = lax.ppermute(out0, "tp", to_chip)
        out1 = project(ho, w_output, wo_other, width - part)
        piece1 = lax.ppermute(out1, "tp", to_chip)
        arrived.append([piece0, piece1])
    total, _, lse_tiles[0] = work(0, width)
    attended = finish(total, sum(arrived, []))

    tiles = []
    for c in range(m):
        for side in range(2):
            at = [lax.rem(c - chip + m, m) == k for k in range(m)]
            ours, theirs = (sum(jnp.where(at[k], lse_tiles[k][i], 0.0) for k in range(m)) for i in range(2))
            tiles.append(jnp.where(core == side, ours, theirs))
    log_total = jnp.stack(tiles).reshape(n_tp * tile_blocks, heads, blk_len)
    log_total = jnp.swapaxes(log_total, 1, 2).reshape(tok_rows, heads)
    return (attended, log_total)


def solution(mesh):
    placed = (P("kv", None), P(None, "tp"), P(), P(), P("tp", None), P("kv", None))
    return jax.shard_map(
        layer,
        mesh=mesh,
        in_specs=placed,
        out_specs=(P(("kv", "tp"), None), P("kv", "tp")),
        check_vma=False,
    )
```
